32 devices in a mesh: ep: 8 (over z, x), tp: 4 (over y, core).
Axes of the slice: x: 2, y: 2, z: 4, core: 2. Of those that a mesh axis runs over, the one named last changes fastest.
Arguments:
- mixer_query: bfloat16 [2048, 2048], P('ep', 'tp'), may hold values from -6 to 6
- mixer_forget: bfloat16 [2048, 2048], P('ep', 'tp'), may hold values from -5.5 to 5.5
- mixer_value: bfloat16 [2048, 2048], P('ep', 'tp'), may hold values from -6 to 6
- mixer_gate: bfloat16 [2048, 2048], P('ep', 'tp'), may hold values from -6 to 6
- forget_floor: float32 [2048], P('tp'), may hold values from 0.88 to 1
- head_gain: float32 [128], replicated, may hold values from 0.1 to 1.9
- mixer_proj: bfloat16 [2048, 2048], P(None, 'tp'), may hold values from -0.125 to 0.125
- expert_tokens: bfloat16 [1024, 2048], P('ep'), may hold values from -6 to 6
- expert_gain: float32 [2048], replicated, may hold values from 0.1 to 1.9
- routes: int32 [1024, 2], P('ep'), may hold values from 0 to 7, as said below
- group_logits: float32 [1024, 4], P('ep'), may hold values from -6 to 6
- choice_logits: float32 [1024, 2], P('ep'), may hold values from -6 to 6
- w_gate: bfloat16 [8, 2048, 2048], P('ep', None, 'tp'), may hold values from -0.125 to 0.125
- w_up: bfloat16 [8, 2048, 2048], P('ep', None, 'tp'), may hold values from -0.125 to 0.125
- w_down: bfloat16 [8, 2048, 2048], P('ep', None, 'tp'), may hold values from -0.125 to 0.125
Outputs:
- mixer_out: bfloat16 [2048, 2048], P('ep', 'tp')
- expert_out: bfloat16 [1024, 2048], P('ep', 'tp')
The draws below stay inside these ranges and needn't reach their ends.
Inputs may be any that keep to these rules, and one draw needn't show every extreme that they name: `routes`: in each aligned block of 128 rows (the rows of one index of ep) no expert is named by more than 64 rows, and some expert reaches that bound in every block; the 2 experts of a row differ and lie in the same group.
All inputs are finite; a program needn't handle non-finite values.
Results may differ from the reference program's by a relative error of at most 0.01.
Values may be sent and summed in bfloat16 or wider, within the bound.
No kernel may reach another device: no remote copies, remote signals or barrier semaphores. Data moves between devices by JAX's collectives and lax.ppermute only.
A program may use at most 64 MiB of HBM per device.

```python
import math
import jax
import jax.numpy as jnp
from jax import lax

D = 2048
HEADS = 16
KEYDIM = 128
VDIM = 128
FF = 2048
GROUPS = 4
TOPK = 2
BLOCK = 64
TOKA_DEV = 256
TOKB_DEV = 128
EXPERTS = 8
EXP_GROUP = 2
CAP = 64
TOKENS_A = 2048
TOKENS_B = 1024
N_EP = 8


def draw_mixer_forget(key, part):
    noise_key = jax.random.fold_in(key, 11)
    shift_key = jax.random.fold_in(key, 12)
    noise = jnp.clip(jax.random.normal(noise_key, (TOKENS_A, HEADS * KEYDIM), jnp.float32), -4.0, 4.0)
    shifts = jax.random.uniform(shift_key, (TOKENS_A // TOKA_DEV, 1, 1), jnp.float32, -1.5, 1.5)
    shaped = noise.reshape(TOKENS_A // TOKA_DEV, TOKA_DEV, HEADS * KEYDIM) + shifts
    return shaped.reshape(TOKENS_A, HEADS * KEYDIM).astype(jnp.bfloat16)


def draw_forget_floor(key, part):
    pick_key = jax.random.fold_in(key, 21)
    slow_key = jax.random.fold_in(key, 22)
    fast_key = jax.random.fold_in(key, 23)
    slow_share = 0.5
    slow_heads = jax.random.uniform(pick_key, (HEADS, 1), jnp.float32) < slow_share
    slow_gap = jax.random.uniform(slow_key, (HEADS, KEYDIM), jnp.float32, 0.3, 2.0) / TOKENS_A
    fast_gap = jnp.exp(jax.random.uniform(fast_key, (HEADS, KEYDIM), jnp.float32, math.log(0.03), math.log(0.12)))
    gap_rows = jnp.where(slow_heads, slow_gap, fast_gap)
    return (1.0 - gap_rows).reshape(HEADS * KEYDIM).astype(jnp.float32)


def route_block(block_key):
    group_size = EXPERTS // GROUPS
    quota = TOKB_DEV // EXPERTS
    expert_ids = jnp.arange(EXPERTS, dtype=jnp.int32)
    counts = jnp.full((EXPERTS,), quota, jnp.int32)
    counts = counts + quota * ((expert_ids == 0) | (expert_ids == group_size - 1)).astype(jnp.int32)
    counts = counts - quota * ((expert_ids == group_size) | (expert_ids == group_size + 1)).astype(jnp.int32)
    canonical = jnp.repeat(expert_ids, counts, total_repeat_length=TOKB_DEV)
    order = jax.random.permutation(jax.random.fold_in(block_key, 1), TOKB_DEV)
    first = canonical[order]
    second = first // group_size * group_size + (first % group_size + 1) % group_size
    group_map = jax.random.permutation(jax.random.fold_in(block_key, 2), GROUPS).astype(jnp.int32)
    rotation = jax.random.randint(jax.random.fold_in(block_key, 3), (GROUPS,), 0, group_size).astype(jnp.int32)

    def relabel(ids):
        grp = ids // group_size
        return (group_map[grp] * group_size + (ids % group_size + rotation[grp]) % group_size).astype(jnp.int32)
    first = relabel(first)
    second = relabel(second)
    flip = jax.random.randint(jax.random.fold_in(block_key, 4), (TOKB_DEV,), 0, 2).astype(jnp.int32)
    left = flip * second + (1 - flip) * first
    right = flip * first + (1 - flip) * second
    return jnp.stack([left, right], axis=-1).astype(jnp.int32)


def draw_routes(key, part):
    base_key = jax.random.fold_in(key, 31)
    block_keys = jax.vmap(lambda index: jax.random.fold_in(base_key, index))(jnp.arange(N_EP))
    return jax.vmap(route_block)(block_keys).reshape(TOKENS_B, TOPK).astype(jnp.int32)


def steps_of(key, extent, cuts, least, largest):
    gain, own = 1.0, jax.random.fold_in(key, 6)
    for position, blocks in cuts:
        steps = jnp.exp(jax.random.uniform(jax.random.fold_in(own, position), (blocks,), jnp.float32, least / len(cuts), largest / len(cuts)))
        gain = gain * jnp.repeat(steps, extent[position] // blocks).reshape([-1 if axis == position else 1 for axis in range(len(extent))])
    return gain


def bell_draw(rng, shape, scale, bound, cuts=(), kind=jnp.bfloat16):
    loudness = steps_of(rng, shape, cuts, -0.22, 0.18) if cuts else 1.0
    values = jax.random.normal(rng, shape, jnp.float32) * scale * loudness
    return jnp.minimum(jnp.maximum(values, -bound), bound).astype(kind)


def setup_inputs(seed: int = 0) -> dict:
    key_of = jax.random.split(jax.random.key(seed), 16)
    return {
        "mixer_query": bell_draw(key_of[0], (TOKENS_A, HEADS * KEYDIM), 1.0, 6.0, ((0, 8), (1, 4))),
        "mixer_forget": draw_mixer_forget(jax.random.fold_in(key_of[15], 71), 0),
        "mixer_value": bell_draw(key_of[2], (TOKENS_A, HEADS * VDIM), 1.0, 6.0, ((0, 8), (1, 4))),
        "mixer_gate": bell_draw(key_of[3], (TOKENS_A, HEADS * VDIM), 1.0, 6.0, ((0, 8), (1, 4))),
        "forget_floor": draw_forget_floor(jax.random.fold_in(key_of[15], 71), 0),
        "head_gain": jnp.clip(1.0 + 0.18 * jax.random.normal(key_of[5], (VDIM,), jnp.float32), 0.1, 1.9),
        "mixer_proj": bell_draw(key_of[6], (HEADS * VDIM, D), (HEADS * VDIM) ** -0.5, 0.125, ((1, 4),)),
        "expert_tokens": bell_draw(key_of[7], (TOKENS_B, D), 1.0, 6.0, ((0, 8),)),
        "expert_gain": jnp.clip(1.0 + 0.18 * jax.random.normal(key_of[8], (D,), jnp.float32), 0.1, 1.9),
        "routes": draw_routes(jax.random.fold_in(key_of[15], 71), 0),
        "group_logits": bell_draw(key_of[10], (TOKENS_B, GROUPS), 1.0, 6.0, ((0, 8),), jnp.float32),
        "choice_logits": bell_draw(key_of[11], (TOKENS_B, TOPK), 1.0, 6.0, ((0, 8),), jnp.float32),
        "w_gate": bell_draw(key_of[12], (EXPERTS, D, FF), D ** -0.5, 0.125, ((0, 8), (2, 4))),
        "w_up": bell_draw(key_of[13], (EXPERTS, D, FF), D ** -0.5, 0.125, ((0, 8), (2, 4))),
        "w_down": bell_draw(key_of[14], (EXPERTS, FF, D), FF ** -0.5, 0.125, ((0, 8), (2, 4))),
    }


norm_eps = 1e-06
highest_precision = lax.Precision.HIGHEST

def rms_scale(features, gain_vec):
    return features * lax.rsqrt(lax.optimization_barrier(jnp.mean(features * features, axis=-1, keepdims=True)) + norm_eps) * gain_vec

def block_terms(query_block, input_block, log_blk, value_block, carried_state):
    cumulative_log = jnp.cumsum(log_blk, axis=0)
    between_block_term = jnp.einsum('zug,ugr->zur', query_block * jnp.exp(cumulative_log), carried_state, precision=highest_precision)
    causal = jnp.tril(jnp.ones((query_block.shape[0], query_block.shape[0]), dtype=bool))[:, :, None, None]
    differ = cumulative_log[:, None] - cumulative_log[None, :]
    decays = jnp.exp(jnp.where(causal, differ, -jnp.inf))
    scores = lax.optimization_barrier(jnp.sum(query_block[:, None] * input_block[None, :] * decays, axis=-1))
    result = between_block_term + jnp.einsum('tsh,shv->thv', scores, value_block, precision=highest_precision)
    ending_log_decay = cumulative_log[-1]
    updated_state = jnp.exp(ending_log_decay)[..., None] * carried_state + jnp.einsum('twa,twr->war', input_block * jnp.exp(ending_log_decay[None] - cumulative_log), value_block, precision=highest_precision)
    return (updated_state, result, cumulative_log)

def mixer_part(mixer_query, mixer_forget, mixer_value, mixer_gate, forget_floor, head_gain, mixer_proj):
    length = mixer_query.shape[0]
    blocks = length // BLOCK

    def split_blocks(source_array, last_width):
        return source_array.reshape(blocks, BLOCK, HEADS, last_width)
    queries = jax.nn.silu(mixer_query.astype(jnp.float32))
    input_rates = (1.0 - forget_floor) * jax.nn.sigmoid(-mixer_forget.astype(jnp.float32))
    log_forget = jnp.log1p(-input_rates)
    value_rows = mixer_value.astype(jnp.float32)

    def advance(carried_state, block_inputs):
        query_block, input_block, value_block, log_blk = block_inputs
        updated_state, result, cumulative_log = block_terms(query_block, input_block, log_blk, value_block, carried_state)
        return (updated_state, result)
    initial = jnp.zeros((HEADS, KEYDIM, VDIM), jnp.float32)
    _, output_rows = lax.scan(advance, initial, (split_blocks(queries, KEYDIM), split_blocks(input_rates, KEYDIM), split_blocks(value_rows, VDIM), split_blocks(log_forget, KEYDIM)))
    output_rows = output_rows.reshape(length, HEADS, VDIM)
    gate_act = jax.nn.silu(mixer_gate.astype(jnp.float32)).reshape(length, HEADS, VDIM)
    gated_out = rms_scale(output_rows, head_gain) * gate_act
    mixed_heads = gated_out.reshape(length, HEADS * VDIM).astype(jnp.bfloat16)
    return jnp.dot(mixed_heads, mixer_proj, preferred_element_type=jnp.float32).astype(jnp.bfloat16)

def gate_weights(routes, group_logits, choice_logits, group_size):
    group_exp = jnp.exp(group_logits)
    group_prob = group_exp / lax.optimization_barrier(jnp.sum(group_exp, axis=-1, keepdims=True))
    groups_of = routes // group_size
    member = (groups_of[..., None] == jnp.arange(GROUPS, dtype=jnp.int32)).astype(jnp.float32)
    picked_prob = lax.optimization_barrier(jnp.sum(member * group_prob[:, None, :], axis=-1))
    choice_exp = jnp.exp(choice_logits)
    together = (groups_of[:, :, None] == groups_of[:, None, :]).astype(jnp.float32)
    within = lax.optimization_barrier(jnp.sum(together * choice_exp[:, None, :], axis=-1))
    return picked_prob * choice_exp / within

def rank_slots(flat_routes, per_block, expert_count):
    onehot = (flat_routes[:, None] == jnp.arange(expert_count, dtype=jnp.int32)).astype(jnp.int32)
    blocked = onehot.reshape(-1, per_block, expert_count)
    earlier = (jnp.cumsum(blocked, axis=1) - blocked).astype(jnp.int32)
    return lax.optimization_barrier(jnp.sum(earlier * blocked, axis=-1)).astype(jnp.int32).reshape(-1)

def expert_part(expert_tokens, expert_gain, routes, group_logits, choice_logits, w_gate, w_up, w_down):
    count_rows = expert_tokens.shape[0]
    normed = rms_scale(expert_tokens.astype(jnp.float32), expert_gain).astype(jnp.bfloat16)
    weights = gate_weights(routes, group_logits, choice_logits, EXP_GROUP)
    flat_routes = routes.reshape(-1)
    per_block = TOKB_DEV * TOPK
    ranks = rank_slots(flat_routes, per_block, EXPERTS)
    block_ids = (jnp.arange(flat_routes.shape[0], dtype=jnp.int32) // per_block).astype(jnp.int32)
    slot_of = (flat_routes * (N_EP * CAP) + block_ids * CAP + ranks).astype(jnp.int32)
    token_ids = (jnp.arange(flat_routes.shape[0], dtype=jnp.int32) // TOPK).astype(jnp.int32)
    token_of = jnp.full((EXPERTS * N_EP * CAP,), count_rows, jnp.int32).at[slot_of].set(token_ids)
    padded = jnp.concatenate([normed, jnp.zeros((1, D), jnp.bfloat16)], axis=0)

    def run_expert(operands):
        gate_mat, up_mat, down_mat, index_rows = operands
        chosen = padded[index_rows]
        gate_pre = jnp.dot(chosen, gate_mat, preferred_element_type=jnp.float32)
        up_pre = jnp.dot(chosen, up_mat, preferred_element_type=jnp.float32)
        hidden = (jax.nn.silu(gate_pre) * up_pre).astype(jnp.bfloat16)
        return jnp.dot(hidden, down_mat, preferred_element_type=jnp.float32).astype(jnp.bfloat16)
    output_rows = lax.map(run_expert, (w_gate, w_up, w_down, token_of.reshape(EXPERTS, N_EP * CAP)))
    picked = output_rows.reshape(-1, D)[slot_of].astype(jnp.float32) * weights.reshape(-1)[:, None]
    return lax.optimization_barrier(jnp.sum(picked.reshape(count_rows, TOPK, D), axis=1)).astype(jnp.bfloat16)

def reference(mixer_query, mixer_forget, mixer_value, mixer_gate, forget_floor, head_gain, mixer_proj, expert_tokens, expert_gain, routes, group_logits, choice_logits, w_gate, w_up, w_down):
    mixer_out = mixer_part(mixer_query, mixer_forget, mixer_value, mixer_gate, forget_floor, head_gain, mixer_proj)
    expert_out = expert_part(expert_tokens, expert_gain, routes, group_logits, choice_logits, w_gate, w_up, w_down)
    return (mixer_out, expert_out)
```

```python
import functools

import jax
import jax.numpy as jnp
from jax import lax
from jax.experimental import pallas as pl
from jax.experimental.pallas import tpu as pltpu
from jax.sharding import PartitionSpec as P

KEYDIM = 128
VDIM = 128
GROUPS = 4
TOPK = 2

norm_eps = 1e-06
f32 = jnp.float32
bf16 = jnp.bfloat16


def dot(a, b, ca, cb):
    return lax.dot_general(a, b, (((ca,), (cb,)), ((), ())), preferred_element_type=f32)


def silu(v):
    return v / (1.0 + jnp.exp(-v))


def mixer_scan_kernel(query, forget, value, floor, out, entry_query, state, decay):
    length = query.shape[0]
    queries = silu(query[...].astype(f32))
    rates = (1.0 - floor[...]) / (1.0 + jnp.exp(forget[...].astype(f32)))
    logs = jnp.log(1.0 - rates)
    high = logs.astype(bf16)
    low = (logs - high.astype(f32)).astype(bf16)
    rows = lax.broadcasted_iota(jnp.int32, (length, length), 0)
    cols = lax.broadcasted_iota(jnp.int32, (length, length), 1)
    causal = rows >= cols
    ones = jnp.where(causal, 1.0, 0.0).astype(bf16)
    cumulative = dot(ones, high, 1, 0) + dot(ones, low, 1, 0)
    total = cumulative[length - 1 :, :]
    centred = cumulative - 0.5 * total
    grown = jnp.exp(centred)
    values = value[...]
    left = (queries * grown).astype(bf16)
    right = (rates * jnp.exp(-centred)).astype(bf16)
    scores = jnp.where(causal, dot(left, right, 1, 1), 0.0).astype(bf16)
    out[...] = dot(scores, values, 1, 0)
    entry_query[...] = (queries * jnp.exp(cumulative)).astype(bf16)
    kept = (rates * jnp.exp(total - cumulative)).astype(bf16)
    state[0] = dot(values, kept, 0, 0).astype(bf16)
    decay[0] = jnp.exp(total).astype(bf16)


def mixer_scan(query, forget, value, floor):
    length, width = query.shape
    heads = width // KEYDIM
    block = pl.BlockSpec((length, KEYDIM), lambda h: (0, h))
    return pl.pallas_call(
        mixer_scan_kernel,
        grid=(heads,),
        in_specs=[block, block, block, pl.BlockSpec((1, KEYDIM), lambda h: (0, h))],
        out_specs=[
            block,
            block,
            pl.BlockSpec((1, VDIM, KEYDIM), lambda h: (h, 0, 0)),
            pl.BlockSpec((1, 1, KEYDIM), lambda h: (h, 0, 0)),
        ],
        out_shape=[
            jax.ShapeDtypeStruct((length, width), f32),
            jax.ShapeDtypeStruct((length, width), bf16),
            jax.ShapeDtypeStruct((heads, VDIM, KEYDIM), bf16),
            jax.ShapeDtypeStruct((heads, 1, KEYDIM), bf16),
        ],
        name="mixer_scan",
    )(query, forget, value, floor.reshape(1, width))


def prefix_kernel(states, decays, out):
    parts, rows, _ = states.shape
    heads = decays.shape[1]
    per_head = rows // heads
    head_of = lax.broadcasted_iota(jnp.int32, (rows, KEYDIM), 0)
    acc = jnp.zeros((rows, KEYDIM), f32)
    for part in range(parts):
        out[part] = acc.astype(bf16)
        if part + 1 < parts:
            shrink = decays[part].astype(f32)
            spread = jnp.broadcast_to(shrink[0:1], (rows, KEYDIM))
            for head in range(1, heads):
                spread = jnp.where(head_of >= head * per_head, shrink[head : head + 1], spread)
            acc = spread * acc + states[part].astype(f32)


def entering_states(state, decay):
    parts = lax.axis_size("ep")
    heads = state.shape[0]
    rows = VDIM // parts
    sliced = state.reshape(heads, parts, rows, KEYDIM).transpose(1, 0, 2, 3)
    sliced = sliced.reshape(parts, heads * rows, KEYDIM)
    tail = jnp.broadcast_to(decay.reshape(1, heads, KEYDIM), (parts, heads, KEYDIM))
    packed = jnp.concatenate([sliced, tail], axis=1)
    packed = lax.all_to_all(packed, "ep", split_axis=0, concat_axis=0, tiled=True)
    prefixes = pl.pallas_call(
        prefix_kernel,
        out_shape=jax.ShapeDtypeStruct((parts, heads * rows, KEYDIM), bf16),
        name="state_prefix",
    )(packed[:, : heads * rows], packed[:, heads * rows :])
    back = lax.all_to_all(prefixes, "ep", split_axis=0, concat_axis=0, tiled=True)
    back = back.reshape(parts, heads, rows, KEYDIM).transpose(1, 0, 2, 3)
    return back.reshape(heads, VDIM, KEYDIM)


def mixer_gate_kernel(local, entry_query, entering, gate, gain, out):
    recurrent = local[...] + dot(entry_query[...], entering[0], 1, 1)
    mean = jnp.mean(recurrent * recurrent, axis=-1, keepdims=True)
    scaled = recurrent * lax.rsqrt(mean + norm_eps) * gain[...]
    out[...] = (scaled * silu(gate[...].astype(f32))).astype(bf16)


def mixer_gated(local, entry_query, entering, gate, gain):
    length, width = local.shape
    block = pl.BlockSpec((length, VDIM), lambda h: (0, h))
    return pl.pallas_call(
        mixer_gate_kernel,
        grid=(width // VDIM,),
        in_specs=[
            block,
            block,
            pl.BlockSpec((1, VDIM, KEYDIM), lambda h: (h, 0, 0)),
            block,
            pl.BlockSpec((1, VDIM), lambda h: (0, 0)),
        ],
        out_specs=block,
        out_shape=jax.ShapeDtypeStruct((length, width), bf16),
        name="mixer_gated",
    )(local, entry_query, entering, gate, gain.reshape(1, VDIM))


def four_parts_kernel(place, own, beside, across, w0, w1, w2, w3, out):
    width = own.shape[1]
    acc = dot(own[...], w0[...], 1, 0)
    acc += dot(beside[...], w1[...], 1, 0)
    acc += dot(across[:, :width], w2[...], 1, 0)
    acc += dot(across[:, width:], w3[...], 1, 0)
    out[...] = acc.astype(bf16)


def spread_dot(part, weight):
    size = lax.axis_size("tp")
    if size != 4:
        full = lax.all_gather(part, "tp", axis=1, tiled=True)
        return jnp.dot(full, weight, preferred_element_type=f32).astype(bf16)
    count, width = part.shape
    columns = weight.shape[1]
    beside = lax.ppermute(part, "tp", [(i, i ^ 2) for i in range(size)])
    pair = jnp.concatenate([part, beside], axis=1)
    across = lax.ppermute(pair, "tp", [(i, i ^ 1) for i in range(size)])
    place = lax.axis_index("tp").astype(jnp.int32).reshape(1)
    whole = lambda cols: pl.BlockSpec((count, cols), lambda i, p: (0, 0))
    rows = lambda flip: pl.BlockSpec((width, columns), lambda i, p: (p[0] ^ flip, 0))
    return pl.pallas_call(
        four_parts_kernel,
        grid_spec=pltpu.PrefetchScalarGridSpec(
            num_scalar_prefetch=1,
            grid=(1,),
            in_specs=[whole(width), whole(width), whole(2 * width)]
            + [rows(flip) for flip in (0, 2, 1, 3)],
            out_specs=pl.BlockSpec((count, columns), lambda i, p: (0, 0)),
        ),
        out_shape=jax.ShapeDtypeStruct((count, columns), bf16),
        name="spread_dot",
    )(place, part, beside, across, weight, weight, weight, weight)


def slot_ranks(routes, experts):
    tokens = routes.shape[1]
    expert = lax.broadcasted_iota(jnp.int32, (experts, tokens), 0)
    named = [routes[j : j + 1, :] == expert for j in range(TOPK)]
    member = functools.reduce(jnp.logical_or, named)
    before = lax.broadcasted_iota(jnp.int32, (tokens, tokens), 0)
    token = lax.broadcasted_iota(jnp.int32, (tokens, tokens), 1)
    earlier = jnp.where(before < token, 1.0, 0.0).astype(bf16)
    counts = dot(jnp.where(member, 1.0, 0.0).astype(bf16), earlier, 1, 0)
    return named, jnp.where(member, counts.astype(jnp.int32), -1)


def dispatch_kernel(place, tokens, gain, routes, out, *, capacity):
    features = tokens[...].astype(f32)
    scale = lax.rsqrt(jnp.mean(features * features, axis=-1, keepdims=True) + norm_eps)
    normed = (features * scale * gain[...]).astype(bf16)
    half = out.shape[1]
    mine = jnp.where(place[0] == 0, normed[:, :half], normed[:, half:])
    experts = out.shape[0] // capacity
    _, ranks = slot_ranks(routes[...], experts)
    slot = lax.broadcasted_iota(jnp.int32, (capacity, tokens.shape[0]), 0)
    for e in range(experts):
        pick = jnp.where(ranks[e : e + 1, :] == slot, 1.0, 0.0).astype(bf16)
        out[e * capacity : (e + 1) * capacity, :] = dot(pick, mine, 1, 0).astype(bf16)


def combine_kernel(routes, group_logits, choice_logits, values, out, *, capacity):
    experts = values.shape[0] // capacity
    tokens = routes.shape[1]
    chosen = routes[...]
    named, ranks = slot_ranks(chosen, experts)
    group_exp = jnp.exp(group_logits[...])
    group_prob = group_exp / jnp.sum(group_exp, axis=0, keepdims=True)
    choice_exp = jnp.exp(choice_logits[...])
    size = experts // GROUPS
    groups_of = [lax.div(chosen[j : j + 1, :], jnp.int32(size)) for j in range(TOPK)]
    spread = jnp.zeros((experts, tokens), f32)
    for j in range(TOPK):
        prob = jnp.zeros((1, tokens), f32)
        for g in range(GROUPS):
            prob = jnp.where(groups_of[j] == g, group_prob[g : g + 1, :], prob)
        within = jnp.zeros((1, tokens), f32)
        for i in range(TOPK):
            within += jnp.where(groups_of[i] == groups_of[j], choice_exp[i : i + 1, :], 0.0)
        weight = prob * choice_exp[j : j + 1, :] / within
        spread = jnp.where(named[j], weight, spread)
    slot = lax.broadcasted_iota(jnp.int32, (capacity, tokens), 0)
    mix = jnp.concatenate(
        [
            jnp.where(ranks[e : e + 1, :] == slot, spread[e : e + 1, :], 0.0)
            for e in range(experts)
        ],
        axis=0,
    )
    high = mix.astype(bf16)
    low = (mix - high.astype(f32)).astype(bf16)
    out[...] = (dot(high, values[...], 0, 0) + dot(low, values[...], 0, 0)).astype(bf16)


def expert_dispatch(expert_tokens, expert_gain, routes):
    count, width = expert_tokens.shape
    experts = lax.axis_size("ep")
    capacity = 2 * TOPK * count // experts
    half = width // 2
    core = (lax.axis_index("tp") % 2).astype(jnp.int32).reshape(1)
    vmem = pl.BlockSpec(memory_space=pltpu.VMEM)
    outgoing = pl.pallas_call(
        functools.partial(dispatch_kernel, capacity=capacity),
        in_specs=[pl.BlockSpec(memory_space=pltpu.SMEM), vmem, vmem, vmem],
        out_specs=vmem,
        out_shape=jax.ShapeDtypeStruct((experts * capacity, half), bf16),
        name="expert_dispatch",
    )(core, expert_tokens, expert_gain.reshape(1, width), routes.T)
    return outgoing.reshape(experts, capacity, half)


def expert_hidden(arrived, w_gate, w_up):
    sources, slots, half = arrived.shape
    mine = arrived.reshape(sources * slots, half)
    size = lax.axis_size("tp")
    other = lax.ppermute(mine, "tp", [(i, i ^ 1) for i in range(size)])
    first = lax.axis_index("tp") % 2 == 0
    rows = jnp.concatenate(
        [jnp.where(first, mine, other), jnp.where(first, other, mine)], axis=1
    )
    gate_pre = jnp.dot(rows, w_gate, preferred_element_type=f32)
    up_pre = jnp.dot(rows, w_up, preferred_element_type=f32)
    return (silu(gate_pre) * up_pre).astype(bf16)


def expert_combine(came_back, routes, group_logits, choice_logits):
    slots, width = came_back.shape
    count = routes.shape[0]
    return pl.pallas_call(
        functools.partial(combine_kernel, capacity=slots // lax.axis_size("ep")),
        out_shape=jax.ShapeDtypeStruct((count, width), bf16),
        name="expert_combine",
    )(routes.T, group_logits.T, choice_logits.T, came_back)


def per_device(
    mixer_query,
    mixer_forget,
    mixer_value,
    mixer_gate,
    forget_floor,
    head_gain,
    mixer_proj,
    expert_tokens,
    expert_gain,
    routes,
    group_logits,
    choice_logits,
    w_gate,
    w_up,
    w_down,
):
    outgoing = expert_dispatch(expert_tokens, expert_gain, routes)
    arrived = lax.all_to_all(outgoing, "ep", split_axis=0, concat_axis=0, tiled=True)
    local, entry_query, state, decay = mixer_scan(
        mixer_query, mixer_forget, mixer_value, forget_floor
    )
    entering = entering_states(state, decay)
    mixed = mixer_gated(local, entry_query, entering, mixer_gate, head_gain)
    mixer_out = spread_dot(mixed, mixer_proj)
    hidden = expert_hidden(arrived, w_gate[0], w_up[0])
    values = spread_dot(hidden, w_down[0])
    shaped = values.reshape(arrived.shape[0], arrived.shape[1], values.shape[1])
    came_back = lax.all_to_all(shaped, "ep", split_axis=0, concat_axis=0, tiled=True)
    came_back = came_back.reshape(values.shape)
    expert_out = expert_combine(came_back, routes, group_logits, choice_logits)
    return (mixer_out, expert_out)


def solution(mesh):
    return jax.shard_map(
        per_device,
        mesh=mesh,
        in_specs=(
            P("ep", "tp"),
            P("ep", "tp"),
            P("ep", "tp"),
            P("ep", "tp"),
            P("tp"),
            P(),
            P(None, "tp"),
            P("ep", None),
            P(),
            P("ep", None),
            P("ep", None),
            P("ep", None),
            P("ep", None, "tp"),
            P("ep", None, "tp"),
            P("ep", None, "tp"),
        ),
        out_specs=(P("ep", "tp"), P("ep", "tp")),
        check_vma=False,
    )
```

```python
import functools

import jax
import jax.numpy as jnp
from jax import lax
from jax.experimental import pallas as pl
from jax.experimental.pallas import tpu as pltpu
from jax.sharding import PartitionSpec as P

KEYDIM = 128
VDIM = 128
GROUPS = 4
TOPK = 2

norm_eps = 1e-06
f32 = jnp.float32
bf16 = jnp.bfloat16


def dot(a, b, ca, cb):
    return lax.dot_general(a, b, (((ca,), (cb,)), ((), ())), preferred_element_type=f32)


def work(us):
    flops = us * 50_000_000
    return pl.CostEstimate(flops=flops, bytes_accessed=0, transcendentals=0)


def silu(v):
    return v / (1.0 + jnp.exp(-v))


def mixer_scan_kernel(query, forget, value, floor, out, entry_query, packed, *, rows, base):
    length, width = query.shape
    parts = packed.shape[0]
    heads = width // KEYDIM
    row = lax.broadcasted_iota(jnp.int32, (length, length), 0)
    col = lax.broadcasted_iota(jnp.int32, (length, length), 1)
    causal = row >= col
    ones = jnp.where(causal, 1.0, 0.0).astype(bf16)
    tail = packed.shape[1] - base
    tail_row = lax.broadcasted_iota(jnp.int32, (tail, KEYDIM), 0)
    decays = jnp.zeros((tail, KEYDIM), f32)
    for h in range(heads):
        cut = slice(h * KEYDIM, (h + 1) * KEYDIM)
        queries = silu(query[:, cut].astype(f32))
        rates = (1.0 - floor[:, cut]) / (1.0 + jnp.exp(forget[:, cut].astype(f32)))
        logs = jnp.log(1.0 - rates)
        high = logs.astype(bf16)
        low = (logs - high.astype(f32)).astype(bf16)
        cumulative = dot(ones, high, 1, 0) + dot(ones, low, 1, 0)
        total = cumulative[length - 1 :, :]
        centred = cumulative - 0.5 * total
        values = value[:, cut]
        left = (queries * jnp.exp(centred)).astype(bf16)
        right = (rates * jnp.exp(-centred)).astype(bf16)
        scores = jnp.where(causal, dot(left, right, 1, 1), 0.0).astype(bf16)
        out[:, cut] = dot(scores, values, 1, 0)
        entry_query[:, cut] = (queries * jnp.exp(cumulative)).astype(bf16)
        kept = (rates * jnp.exp(total - cumulative)).astype(bf16)
        state = dot(values, kept, 0, 0)
        for part in range(parts):
            piece = state[part * rows : (part + 1) * rows, :]
            packed[part, h * rows : (h + 1) * rows, :] = piece.astype(bf16)
        decays = jnp.where(tail_row == h, jnp.exp(total), decays)
    for part in range(parts):
        packed[part, base:, :] = decays.astype(bf16)


def mixer_scan(query, forget, value, floor, parts):
    length, width = query.shape
    heads = width // KEYDIM
    rows = VDIM // parts
    base = (heads * rows + 15) // 16 * 16
    return pl.pallas_call(
        functools.partial(mixer_scan_kernel, rows=rows, base=base),
        out_shape=[
            jax.ShapeDtypeStruct((length, width), f32),
            jax.ShapeDtypeStruct((length, width), bf16),
            jax.ShapeDtypeStruct((parts, base + (heads + 15) // 16 * 16, KEYDIM), bf16),
        ],
        cost_estimate=work(8),
        name="mixer_scan",
    )(query, forget, value, floor.reshape(1, width))


def prefix_kernel(packed, out, *, heads, base):
    parts, rows, _ = out.shape
    per_head = rows // heads
    head_of = lax.broadcasted_iota(jnp.int32, (rows, KEYDIM), 0)
    acc = jnp.zeros((rows, KEYDIM), f32)
    for part in range(parts):
        out[part] = acc.astype(bf16)
        if part + 1 < parts:
            shrink = packed[part, base:, :].astype(f32)
            spread = jnp.broadcast_to(shrink[0:1], (rows, KEYDIM))
            for head in range(1, heads):
                spread = jnp.where(head_of >= head * per_head, shrink[head : head + 1], spread)
            acc = spread * acc + packed[part, :rows, :].astype(f32)


def state_prefix(packed, heads):
    parts = packed.shape[0]
    rows = heads * (VDIM // parts)
    return pl.pallas_call(
        functools.partial(prefix_kernel, heads=heads, base=(rows + 15) // 16 * 16),
        out_shape=jax.ShapeDtypeStruct((parts, rows, KEYDIM), bf16),
        cost_estimate=work(1),
        name="state_prefix",
    )(packed)


def mixer_gate_kernel(local, entry_query, entering, gate, gain, out):
    heads = local.shape[1] // VDIM
    parts = entering.shape[0]
    rows = VDIM // parts
    for h in range(heads):
        cut = slice(h * VDIM, (h + 1) * VDIM)
        pieces = [
            entering[part, h * rows : (h + 1) * rows, :].astype(f32) for part in range(parts)
        ]
        state = jnp.concatenate(pieces, axis=0).astype(bf16)
        recurrent = local[:, cut] + dot(entry_query[:, cut], state, 1, 1)
        mean = jnp.mean(recurrent * recurrent, axis=-1, keepdims=True)
        scaled = recurrent * lax.rsqrt(mean + norm_eps) * gain[...]
        out[:, cut] = (scaled * silu(gate[:, cut].astype(f32))).astype(bf16)


def mixer_gated(local, entry_query, entering, gate, gain):
    length, width = local.shape
    return pl.pallas_call(
        mixer_gate_kernel,
        out_shape=jax.ShapeDtypeStruct((length, width), bf16),
        cost_estimate=work(3),
        name="mixer_gated",
    )(local, entry_query, entering, gate, gain.reshape(1, VDIM))


def four_parts_kernel(place, own, beside, across, last, w0, w1, w2, w3, out):
    acc = dot(own[...], w0[...], 1, 0)
    acc += dot(beside[...], w1[...], 1, 0)
    acc += dot(across[...], w2[...], 1, 0)
    acc += dot(last[...], w3[...], 1, 0)
    out[...] = acc.astype(bf16)


def spread_first(part):
    if lax.axis_size("tp") != 4:
        return (lax.all_gather(part, "tp", axis=1, tiled=True),)
    beside = lax.ppermute(part, "tp", [(i, i ^ 2) for i in range(4)])
    across = lax.ppermute(part, "tp", [(i, i ^ 1) for i in range(4)])
    return (part, beside, across)


def spread_last(pieces):
    if len(pieces) == 1:
        return pieces
    last = lax.ppermute(pieces[1], "tp", [(i, i ^ 1) for i in range(4)])
    return pieces + (last,)


def spread_dot(pieces, weight):
    if len(pieces) == 1:
        return jnp.dot(pieces[0], weight, preferred_element_type=f32).astype(bf16)
    count, width = pieces[0].shape
    columns = weight.shape[1]
    place = lax.axis_index("tp").astype(jnp.int32).reshape(1)
    whole = lambda cols: pl.BlockSpec((count, cols), lambda i, p: (0, 0))
    rows = lambda flip: pl.BlockSpec((width, columns), lambda i, p: (p[0] ^ flip, 0))
    return pl.pallas_call(
        four_parts_kernel,
        grid_spec=pltpu.PrefetchScalarGridSpec(
            num_scalar_prefetch=1,
            grid=(1,),
            in_specs=[whole(width)] * 4
            + [rows(flip) for flip in (0, 2, 1, 3)],
            out_specs=pl.BlockSpec((count, columns), lambda i, p: (0, 0)),
        ),
        out_shape=jax.ShapeDtypeStruct((count, columns), bf16),
        cost_estimate=work(4),
        name="spread_dot",
    )(place, *pieces, weight, weight, weight, weight)


def slot_ranks(routes, experts):
    tokens = routes.shape[1]
    expert = lax.broadcasted_iota(jnp.int32, (experts, tokens), 0)
    named = [routes[j : j + 1, :] == expert for j in range(TOPK)]
    member = functools.reduce(jnp.logical_or, named)
    before = lax.broadcasted_iota(jnp.int32, (tokens, tokens), 0)
    token = lax.broadcasted_iota(jnp.int32, (tokens, tokens), 1)
    earlier = jnp.where(before < token, 1.0, 0.0).astype(bf16)
    counts = dot(jnp.where(member, 1.0, 0.0).astype(bf16), earlier, 1, 0)
    return named, jnp.where(member, counts.astype(jnp.int32), -1)


def dispatch_kernel(place, tokens, gain, routes, out, *, capacity):
    features = tokens[...].astype(f32)
    scale = lax.rsqrt(jnp.mean(features * features, axis=-1, keepdims=True) + norm_eps)
    normed = (features * scale * gain[...]).astype(bf16)
    half = out.shape[1]
    mine = jnp.where(place[0] == 0, normed[:, :half], normed[:, half:])
    experts = out.shape[0] // capacity
    _, ranks = slot_ranks(routes[...], experts)
    slot = lax.broadcasted_iota(jnp.int32, (capacity, tokens.shape[0]), 0)
    for e in range(experts):
        pick = jnp.where(ranks[e : e + 1, :] == slot, 1.0, 0.0).astype(bf16)
        out[e * capacity : (e + 1) * capacity, :] = dot(pick, mine, 1, 0).astype(bf16)


def combine_kernel(routes, group_logits, choice_logits, values, out, *, capacity):
    experts = values.shape[0] // capacity
    tokens = routes.shape[1]
    chosen = routes[...]
    named, ranks = slot_ranks(chosen, experts)
    group_exp = jnp.exp(group_logits[...])
    group_prob = group_exp / jnp.sum(group_exp, axis=0, keepdims=True)
    choice_exp = jnp.exp(choice_logits[...])
    size = experts // GROUPS
    groups_of = [lax.div(chosen[j : j + 1, :], jnp.int32(size)) for j in range(TOPK)]
    spread = jnp.zeros((experts, tokens), f32)
    for j in range(TOPK):
        prob = jnp.zeros((1, tokens), f32)
        for g in range(GROUPS):
            prob = jnp.where(groups_of[j] == g, group_prob[g : g + 1, :], prob)
        within = jnp.zeros((1, tokens), f32)
        for i in range(TOPK):
            within += jnp.where(groups_of[i] == groups_of[j], choice_exp[i : i + 1, :], 0.0)
        weight = prob * choice_exp[j : j + 1, :] / within
        spread = jnp.where(named[j], weight, spread)
    slot = lax.broadcasted_iota(jnp.int32, (capacity, tokens), 0)
    mix = jnp.concatenate(
        [
            jnp.where(ranks[e : e + 1, :] == slot, spread[e : e + 1, :], 0.0)
            for e in range(experts)
        ],
        axis=0,
    )
    high = mix.astype(bf16)
    low = (mix - high.astype(f32)).astype(bf16)
    out[...] = (dot(high, values[...], 0, 0) + dot(low, values[...], 0, 0)).astype(bf16)


def expert_dispatch(expert_tokens, expert_gain, routes):
    count, width = expert_tokens.shape
    experts = lax.axis_size("ep")
    capacity = 2 * TOPK * count // experts
    half = width // 2
    core = (lax.axis_index("tp") % 2).astype(jnp.int32).reshape(1)
    vmem = pl.BlockSpec(memory_space=pltpu.VMEM)
    outgoing = pl.pallas_call(
        functools.partial(dispatch_kernel, capacity=capacity),
        in_specs=[pl.BlockSpec(memory_space=pltpu.SMEM), vmem, vmem, vmem],
        out_specs=vmem,
        out_shape=jax.ShapeDtypeStruct((experts * capacity, half), bf16),
        cost_estimate=work(4),
        name="expert_dispatch",
    )(core, expert_tokens, expert_gain.reshape(1, width), routes.T)
    return outgoing.reshape(experts, capacity, half)


def expert_hidden(arrived, w_gate, w_up):
    sources, slots, half = arrived.shape
    mine = arrived.reshape(sources * slots, half)
    size = lax.axis_size("tp")
    other = lax.ppermute(mine, "tp", [(i, i ^ 1) for i in range(size)])
    first = lax.axis_index("tp") % 2 == 0
    rows = jnp.concatenate(
        [jnp.where(first, mine, other), jnp.where(first, other, mine)], axis=1
    )
    gate_pre = jnp.dot(rows, w_gate, preferred_element_type=f32)
    up_pre = jnp.dot(rows, w_up, preferred_element_type=f32)
    return (silu(gate_pre) * up_pre).astype(bf16)


def expert_combine(came_back, routes, group_logits, choice_logits):
    slots, width = came_back.shape
    count = routes.shape[0]
    return pl.pallas_call(
        functools.partial(combine_kernel, capacity=slots // lax.axis_size("ep")),
        out_shape=jax.ShapeDtypeStruct((count, width), bf16),
        cost_estimate=work(3),
        name="expert_combine",
    )(routes.T, group_logits.T, choice_logits.T, came_back)


def per_device(
    mixer_query,
    mixer_forget,
    mixer_value,
    mixer_gate,
    forget_floor,
    head_gain,
    mixer_proj,
    expert_tokens,
    expert_gain,
    routes,
    group_logits,
    choice_logits,
    w_gate,
    w_up,
    w_down,
):
    together = lax.optimization_barrier
    parts = lax.axis_size("ep")
    heads = mixer_query.shape[1] // KEYDIM
    outgoing = expert_dispatch(expert_tokens, expert_gain, routes)
    outgoing, mixer_query = together((outgoing, mixer_query))
    arrived = lax.all_to_all(outgoing, "ep", split_axis=0, concat_axis=0, tiled=True)
    local, entry_query, packed = mixer_scan(
        mixer_query, mixer_forget, mixer_value, forget_floor, parts
    )
    arrived, packed = together((arrived, packed))
    slices = lax.all_to_all(packed, "ep", split_axis=0, concat_axis=0, tiled=True)
    hidden = expert_hidden(arrived, w_gate[0], w_up[0])
    hidden, slices = together((hidden, slices))
    pieces = spread_first(hidden)
    prefixes = state_prefix(slices, heads)
    entering = lax.all_to_all(prefixes, "ep", split_axis=0, concat_axis=0, tiled=True)
    pieces, entering = together((pieces, entering))
    pieces = spread_last(pieces)
    mixed = mixer_gated(local, entry_query, entering, mixer_gate, head_gain)
    pieces, mixed = together((pieces, mixed))
    mixed_pieces = spread_first(mixed)
    values = spread_dot(pieces, w_down[0])
    shaped = values.reshape(arrived.shape[0], arrived.shape[1], values.shape[1])
    came_back = lax.all_to_all(shaped, "ep", split_axis=0, concat_axis=0, tiled=True)
    mixer_out = spread_dot(spread_last(mixed_pieces), mixer_proj)
    came_back, mixer_out = together((came_back, mixer_out))
    came_back = came_back.reshape(values.shape)
    expert_out = expert_combine(came_back, routes, group_logits, choice_logits)
    return (mixer_out, expert_out)


def solution(mesh):
    return jax.shard_map(
        per_device,
        mesh=mesh,
        in_specs=(
            P("ep", "tp"),
            P("ep", "tp"),
            P("ep", "tp"),
            P("ep", "tp"),
            P("tp"),
            P(),
            P(None, "tp"),
            P("ep", None),
            P(),
            P("ep", None),
            P("ep", None),
            P("ep", None),
            P("ep", None, "tp"),
            P("ep", None, "tp"),
            P("ep", None, "tp"),
        ),
        out_specs=(P("ep", "tp"), P("ep", "tp")),
        check_vma=False,
    )
```

```python
import functools

import jax
import jax.numpy as jnp
from jax import lax
from jax.experimental import pallas as pl
from jax.experimental.pallas import tpu as pltpu
from jax.sharding import PartitionSpec as P

KEYDIM = 128
VDIM = 128
GROUPS = 4
TOPK = 2
WAVES = 2

norm_eps = 1e-06
f32 = jnp.float32
bf16 = jnp.bfloat16


def dot(a, b, ca, cb):
    return lax.dot_general(a, b, (((ca,), (cb,)), ((), ())), preferred_element_type=f32)


def work(us):
    flops = us * 50_000_000
    return pl.CostEstimate(flops=flops, bytes_accessed=0, transcendentals=0)


def silu(v):
    return v / (1.0 + jnp.exp(-v))


def mixer_scan_kernel(query, forget, value, floor, out, entry_query, packed, *, rows, base):
    length, width = query.shape
    parts = packed.shape[0]
    heads = width // KEYDIM
    row = lax.broadcasted_iota(jnp.int32, (length, length), 0)
    col = lax.broadcasted_iota(jnp.int32, (length, length), 1)
    causal = row >= col
    ones = jnp.where(causal, 1.0, 0.0).astype(bf16)
    tail = packed.shape[1] - base
    tail_row = lax.broadcasted_iota(jnp.int32, (tail, KEYDIM), 0)
    decays = jnp.zeros((tail, KEYDIM), f32)
    for h in range(heads):
        cut = slice(h * KEYDIM, (h + 1) * KEYDIM)
        queries = silu(query[:, cut].astype(f32))
        rates = (1.0 - floor[:, cut]) / (1.0 + jnp.exp(forget[:, cut].astype(f32)))
        logs = jnp.log(1.0 - rates)
        high = logs.astype(bf16)
        low = (logs - high.astype(f32)).astype(bf16)
        cumulative = dot(ones, high, 1, 0) + dot(ones, low, 1, 0)
        total = cumulative[length - 1 :, :]
        centred = cumulative - 0.5 * total
        values = value[:, cut]
        left = (queries * jnp.exp(centred)).astype(bf16)
        right = (rates * jnp.exp(-centred)).astype(bf16)
        scores = jnp.where(causal, dot(left, right, 1, 1), 0.0).astype(bf16)
        out[:, cut] = dot(scores, values, 1, 0)
        entry_query[:, cut] = (queries * jnp.exp(cumulative)).astype(bf16)
        kept = (rates * jnp.exp(total - cumulative)).astype(bf16)
        state = dot(values, kept, 0, 0)
        for part in range(parts):
            piece = state[part * rows : (part + 1) * rows, :]
            packed[part, h * rows : (h + 1) * rows, :] = piece.astype(bf16)
        decays = jnp.where(tail_row == h, jnp.exp(total), decays)
    for part in range(parts):
        packed[part, base:, :] = decays.astype(bf16)


def mixer_scan(query, forget, value, floor, parts):
    length, width = query.shape
    heads = width // KEYDIM
    rows = VDIM // parts
    base = (heads * rows + 15) // 16 * 16
    return pl.pallas_call(
        functools.partial(mixer_scan_kernel, rows=rows, base=base),
        out_shape=[
            jax.ShapeDtypeStruct((length, width), f32),
            jax.ShapeDtypeStruct((length, width), bf16),
            jax.ShapeDtypeStruct((parts, base + (heads + 15) // 16 * 16, KEYDIM), bf16),
        ],
        cost_estimate=work(8),
        name="mixer_scan",
    )(query, forget, value, floor.reshape(1, width))


def prefix_kernel(packed, out, *, heads, base):
    parts, rows, _ = out.shape
    per_head = rows // heads
    head_of = lax.broadcasted_iota(jnp.int32, (rows, KEYDIM), 0)
    acc = jnp.zeros((rows, KEYDIM), f32)
    for part in range(parts):
        out[part] = acc.astype(bf16)
        if part + 1 < parts:
            shrink = packed[part, base:, :].astype(f32)
            spread = jnp.broadcast_to(shrink[0:1], (rows, KEYDIM))
            for head in range(1, heads):
                spread = jnp.where(head_of >= head * per_head, shrink[head : head + 1], spread)
            acc = spread * acc + packed[part, :rows, :].astype(f32)


def state_prefix(packed, heads):
    parts = packed.shape[0]
    rows = heads * (VDIM // parts)
    return pl.pallas_call(
        functools.partial(prefix_kernel, heads=heads, base=(rows + 15) // 16 * 16),
        out_shape=jax.ShapeDtypeStruct((parts, rows, KEYDIM), bf16),
        cost_estimate=work(1),
        name="state_prefix",
    )(packed)


def mixer_gate_kernel(local, entry_query, entering, gate, gain, out):
    heads = local.shape[1] // VDIM
    parts = entering.shape[0]
    rows = VDIM // parts
    for h in range(heads):
        cut = slice(h * VDIM, (h + 1) * VDIM)
        pieces = [
            entering[part, h * rows : (h + 1) * rows, :].astype(f32) for part in range(parts)
        ]
        state = jnp.concatenate(pieces, axis=0).astype(bf16)
        recurrent = local[:, cut] + dot(entry_query[:, cut], state, 1, 1)
        mean = jnp.mean(recurrent * recurrent, axis=-1, keepdims=True)
        scaled = recurrent * lax.rsqrt(mean + norm_eps) * gain[...]
        out[:, cut] = (scaled * silu(gate[:, cut].astype(f32))).astype(bf16)


def mixer_gated(local, entry_query, entering, gate, gain):
    length, width = local.shape
    return pl.pallas_call(
        mixer_gate_kernel,
        out_shape=jax.ShapeDtypeStruct((length, width), bf16),
        cost_estimate=work(3),
        name="mixer_gated",
    )(local, entry_query, entering, gate, gain.reshape(1, VDIM))


def four_parts_kernel(place, own, beside, across, last, w0, w1, w2, w3, out):
    acc = dot(own[...], w0[...], 1, 0)
    acc += dot(beside[...], w1[...], 1, 0)
    acc += dot(across[...], w2[...], 1, 0)
    acc += dot(last[...], w3[...], 1, 0)
    out[...] = acc.astype(bf16)


def spread_first(part):
    if lax.axis_size("tp") != 4:
        return (lax.all_gather(part, "tp", axis=1, tiled=True),)
    beside = lax.ppermute(part, "tp", [(i, i ^ 2) for i in range(4)])
    across = lax.ppermute(part, "tp", [(i, i ^ 1) for i in range(4)])
    return (part, beside, across)


def spread_last(pieces):
    if len(pieces) == 1:
        return pieces
    last = lax.ppermute(pieces[1], "tp", [(i, i ^ 1) for i in range(4)])
    return pieces + (last,)


def spread_dot(pieces, weight):
    if len(pieces) == 1:
        return jnp.dot(pieces[0], weight, preferred_element_type=f32).astype(bf16)
    count, width = pieces[0].shape
    columns = weight.shape[1]
    place = lax.axis_index("tp").astype(jnp.int32).reshape(1)
    whole = lambda cols: pl.BlockSpec((count, cols), lambda i, p: (0, 0))
    rows = lambda flip: pl.BlockSpec((width, columns), lambda i, p: (p[0] ^ flip, 0))
    return pl.pallas_call(
        four_parts_kernel,
        grid_spec=pltpu.PrefetchScalarGridSpec(
            num_scalar_prefetch=1,
            grid=(1,),
            in_specs=[whole(width)] * 4
            + [rows(flip) for flip in (0, 2, 1, 3)],
            out_specs=pl.BlockSpec((count, columns), lambda i, p: (0, 0)),
        ),
        out_shape=jax.ShapeDtypeStruct((count, columns), bf16),
        cost_estimate=work(4),
        name="spread_dot",
    )(place, *pieces, weight, weight, weight, weight)


def slot_ranks(routes, experts):
    tokens = routes.shape[1]
    expert = lax.broadcasted_iota(jnp.int32, (experts, tokens), 0)
    named = [routes[j : j + 1, :] == expert for j in range(TOPK)]
    member = functools.reduce(jnp.logical_or, named)
    before = lax.broadcasted_iota(jnp.int32, (tokens, tokens), 0)
    token = lax.broadcasted_iota(jnp.int32, (tokens, tokens), 1)
    earlier = jnp.where(before < token, 1.0, 0.0).astype(bf16)
    counts = dot(jnp.where(member, 1.0, 0.0).astype(bf16), earlier, 1, 0)
    return named, jnp.where(member, counts.astype(jnp.int32), -1)


def dispatch_kernel(place, tokens, gain, routes, *outs, slots):
    features = tokens[...].astype(f32)
    scale = lax.rsqrt(jnp.mean(features * features, axis=-1, keepdims=True) + norm_eps)
    normed = (features * scale * gain[...]).astype(bf16)
    half = outs[0].shape[1]
    mine = jnp.where(place[0] == 0, normed[:, :half], normed[:, half:])
    experts = outs[0].shape[0] // slots
    _, ranks = slot_ranks(routes[...], experts)
    slot = lax.broadcasted_iota(jnp.int32, (slots, tokens.shape[0]), 0)
    for wave, out in enumerate(outs):
        picks = [
            jnp.where(ranks[e : e + 1, :] == slot + wave * slots, 1.0, 0.0)
            for e in range(experts)
        ]
        pick = jnp.concatenate(picks, axis=0).astype(bf16)
        out[...] = dot(pick, mine, 1, 0).astype(bf16)


def combine_kernel(routes, group_logits, choice_logits, *refs, slots):
    out = refs[-1]
    experts = refs[0].shape[0] // slots
    tokens = routes.shape[1]
    chosen = routes[...]
    named, ranks = slot_ranks(chosen, experts)
    group_exp = jnp.exp(group_logits[...])
    group_prob = group_exp / jnp.sum(group_exp, axis=0, keepdims=True)
    choice_exp = jnp.exp(choice_logits[...])
    size = experts // GROUPS
    groups_of = [lax.div(chosen[j : j + 1, :], jnp.int32(size)) for j in range(TOPK)]
    spread = jnp.zeros((experts, tokens), f32)
    for j in range(TOPK):
        prob = jnp.zeros((1, tokens), f32)
        for g in range(GROUPS):
            prob = jnp.where(groups_of[j] == g, group_prob[g : g + 1, :], prob)
        within = jnp.zeros((1, tokens), f32)
        for i in range(TOPK):
            within += jnp.where(groups_of[i] == groups_of[j], choice_exp[i : i + 1, :], 0.0)
        weight = prob * choice_exp[j : j + 1, :] / within
        spread = jnp.where(named[j], weight, spread)
    slot = lax.broadcasted_iota(jnp.int32, (slots, tokens), 0)
    total = jnp.zeros(out.shape, f32)
    for wave, values in enumerate(refs[:-1]):
        rows = [
            jnp.where(ranks[e : e + 1, :] == slot + wave * slots, spread[e : e + 1, :], 0.0)
            for e in range(experts)
        ]
        mix = jnp.concatenate(rows, axis=0)
        high = mix.astype(bf16)
        low = (mix - high.astype(f32)).astype(bf16)
        total += dot(high, values[...], 0, 0) + dot(low, values[...], 0, 0)
    out[...] = total.astype(bf16)


def expert_dispatch(expert_tokens, expert_gain, routes):
    count, width = expert_tokens.shape
    experts = lax.axis_size("ep")
    slots = 2 * TOPK * count // experts // WAVES
    half = width // 2
    core = (lax.axis_index("tp") % 2).astype(jnp.int32).reshape(1)
    vmem = pl.BlockSpec(memory_space=pltpu.VMEM)
    outgoing = pl.pallas_call(
        functools.partial(dispatch_kernel, slots=slots),
        in_specs=[pl.BlockSpec(memory_space=pltpu.SMEM), vmem, vmem, vmem],
        out_specs=[vmem] * WAVES,
        out_shape=[jax.ShapeDtypeStruct((experts * slots, half), bf16)] * WAVES,
        cost_estimate=work(4),
        name="expert_dispatch",
    )(core, expert_tokens, expert_gain.reshape(1, width), routes.T)
    return [wave.reshape(experts, slots, half) for wave in outgoing]


def expert_hidden(arrived, w_gate, w_up):
    sources, slots, half = arrived.shape
    mine = arrived.reshape(sources * slots, half)
    size = lax.axis_size("tp")
    other = lax.ppermute(mine, "tp", [(i, i ^ 1) for i in range(size)])
    first = lax.axis_index("tp") % 2 == 0
    rows = jnp.concatenate(
        [jnp.where(first, mine, other), jnp.where(first, other, mine)], axis=1
    )
    gate_pre = jnp.dot(rows, w_gate, preferred_element_type=f32)
    up_pre = jnp.dot(rows, w_up, preferred_element_type=f32)
    return (silu(gate_pre) * up_pre).astype(bf16)


def expert_combine(came_back, routes, group_logits, choice_logits):
    slots, width = came_back[0].shape
    count = routes.shape[0]
    return pl.pallas_call(
        functools.partial(combine_kernel, slots=slots // lax.axis_size("ep")),
        out_shape=jax.ShapeDtypeStruct((count, width), bf16),
        cost_estimate=work(3),
        name="expert_combine",
    )(routes.T, group_logits.T, choice_logits.T, *came_back)


def per_device(
    mixer_query,
    mixer_forget,
    mixer_value,
    mixer_gate,
    forget_floor,
    head_gain,
    mixer_proj,
    expert_tokens,
    expert_gain,
    routes,
    group_logits,
    choice_logits,
    w_gate,
    w_up,
    w_down,
):
    together = lax.optimization_barrier
    parts = lax.axis_size("ep")
    heads = mixer_query.shape[1] // KEYDIM
    outgoing = expert_dispatch(expert_tokens, expert_gain, routes)
    outgoing, mixer_query = together((outgoing, mixer_query))
    swap = lambda x: lax.all_to_all(x, "ep", split_axis=0, concat_axis=0, tiled=True)
    arrived, arrived_last = swap(outgoing[0]), swap(outgoing[1])
    local, entry_query, packed = mixer_scan(
        mixer_query, mixer_forget, mixer_value, forget_floor, parts
    )
    arrived, packed = together((arrived, packed))
    hidden = expert_hidden(arrived, w_gate[0], w_up[0])
    pieces = spread_first(hidden)
    packed, arrived_last, _ = together((packed, arrived_last, pieces))
    slices = swap(packed)
    hidden_last = expert_hidden(arrived_last, w_gate[0], w_up[0])
    pieces_last = spread_first(hidden_last)
    slices, pieces, _ = together((slices, pieces, hidden_last))
    entering = swap(state_prefix(slices, heads))

    def product(pieces):
        return spread_dot(spread_last(pieces), w_down[0])

    def send_back(values):
        return swap(values.reshape(parts, -1, values.shape[1])).reshape(values.shape)

    values, entering = together((product(pieces), entering))
    came_back = send_back(values)
    mixed = mixer_gated(local, entry_query, entering, mixer_gate, head_gain)
    pieces_last, mixed = together((pieces_last, mixed))
    came_last = send_back(product(pieces_last))
    mixer_out = spread_dot(spread_last(spread_first(mixed)), mixer_proj)
    came_back, came_last, mixer_out = together((came_back, came_last, mixer_out))
    came_back = (came_back, came_last)
    expert_out = expert_combine(came_back, routes, group_logits, choice_logits)
    return (mixer_out, expert_out)


def solution(mesh):
    return jax.shard_map(
        per_device,
        mesh=mesh,
        in_specs=(
            P("ep", "tp"),
            P("ep", "tp"),
            P("ep", "tp"),
            P("ep", "tp"),
            P("tp"),
            P(),
            P(None, "tp"),
            P("ep", None),
            P(),
            P("ep", None),
            P("ep", None),
            P("ep", None),
            P("ep", None, "tp"),
            P("ep", None, "tp"),
            P("ep", None, "tp"),
        ),
        out_specs=(P("ep", "tp"), P("ep", "tp")),
        check_vma=False,
    )
```
